32 devices in a mesh: kv: 8 (over z, y), tp: 4 (over x, core).
Axes of the slice: x: 2, y: 2, z: 4, core: 2. Of those that a mesh axis runs over, the one named last changes fastest.
Arguments:
- residual: bfloat16 [256, 2048], P('kv', 'tp'), may hold values from -12 to 12
- first_gain: bfloat16 [2048], P('tp'), may hold values from 0.099609375 to 1.8984375
- first_gate: bfloat16 [2048, 5632], P('tp', 'kv'), may hold values from -0.125 to 0.125
- first_lift: bfloat16 [2048, 5632], P('tp', 'kv'), may hold values from -0.125 to 0.125
- first_down: bfloat16 [5632, 2048], P('kv', 'tp'), may hold values from -0.078125 to 0.078125
- mixer_gain: bfloat16 [2048], replicated, may hold values from 0.099609375 to 1.8984375
- proj_gate: bfloat16 [2048, 2048], P(None, 'tp'), may hold values from -0.125 to 0.125
- proj_input: bfloat16 [2048, 2048], P(None, 'tp'), may hold values from -0.125 to 0.125
- proj_write: bfloat16 [2048, 1024], P(None, 'tp'), may hold values from -0.125 to 0.125
- proj_read: bfloat16 [2048, 1024], P(None, 'tp'), may hold values from -0.125 to 0.125
- proj_step: bfloat16 [2048, 32], P(None, 'tp'), may hold values from -0.125 to 0.125
- step_bias: float32 [32], P('tp'), may hold values from -5 to -2
- rate_log: float32 [32], P('tp'), may hold values from -0.7 to 2.1
- skip_gain: float32 [32], P('tp'), may hold values from 0.5 to 2
- taps_input: bfloat16 [4, 2048], P(None, 'tp'), may hold values from -3 to 3
- taps_write: bfloat16 [4, 1024], P(None, 'tp'), may hold values from -3 to 3
- taps_read: bfloat16 [4, 1024], P(None, 'tp'), may hold values from -3 to 3
- buffer_input: bfloat16 [256, 3, 2048], P('kv', None, 'tp'), may hold values from -6 to 6
- buffer_write: bfloat16 [256, 3, 1024], P('kv', None, 'tp'), may hold values from -6 to 6
- buffer_read: bfloat16 [256, 3, 1024], P('kv', None, 'tp'), may hold values from -6 to 6
- scan_state: float32 [256, 32, 64, 128], P('kv', 'tp'), may hold values from -1.5 to 1.5
- group_gain: bfloat16 [2048], P('tp'), may hold values from 0.099609375 to 1.8984375
- proj_output: bfloat16 [2048, 2048], P('tp'), may hold values from -0.125 to 0.125
- second_gain: bfloat16 [2048], P('tp'), may hold values from 0.099609375 to 1.8984375
- second_gate: bfloat16 [2048, 5632], P('tp', 'kv'), may hold values from -0.125 to 0.125
- second_lift: bfloat16 [2048, 5632], P('tp', 'kv'), may hold values from -0.125 to 0.125
- second_down: bfloat16 [5632, 2048], P('kv', 'tp'), may hold values from -0.078125 to 0.078125
Outputs:
- residual_out: bfloat16 [256, 2048], P('kv', 'tp')
- state_out: float32 [256, 32, 64, 128], P('kv', 'tp')
The draws below stay inside these ranges and needn't reach their ends.
All inputs are finite; a program needn't handle non-finite values.
Results may differ from the reference program's by a relative error of at most 0.023.
Values may be sent and summed in bfloat16 or wider, within the bound.
A program may use at most 64 MiB of HBM per device.

```python
import jax
import jax.numpy as jnp
from jax import lax

D = 2048
FF = 5632
HEADS = 32
HEAD_DIM = 64
STATE = 128
NGROUPS = 8
CONV = 4
D_SSD = 2048
BATCH = 256
N_TP = 4


def draw_residual(key, part):
    first_key = jax.random.fold_in(key, 0)
    columns = jnp.arange(D, dtype=jnp.float32)
    column_ramp = 0.5 * jnp.power(4.0, columns / (D - 1))
    entries = jax.random.normal(first_key, (BATCH, D), jnp.float32)
    return jnp.clip(entries * column_ramp[None, :], -12.0, 12.0).astype(jnp.bfloat16)


def steps_of(own_key, extent, cuts, least, largest):
    level, own = 1.0, jax.random.fold_in(own_key, 6)
    for position, shards_of in cuts:
        heights = jnp.exp(jax.random.uniform(jax.random.fold_in(own, position), (shards_of,), jnp.float32, least / len(cuts), largest / len(cuts)))
        level = level * jnp.repeat(heights, extent[position] // shards_of).reshape([-1 if axis == position else 1 for axis in range(len(extent))])
    return level


def gaussian(key, dims, width, most, shards=(), held_as=jnp.bfloat16):
    level = steps_of(key, dims, shards, -0.22, 0.18) if shards else 1.0
    values = jax.random.normal(key, dims, jnp.float32) * width * level
    return jnp.minimum(jnp.maximum(values, -most), most).astype(held_as)


def setup_inputs(seed: int = 0) -> dict:
    seeds = jax.random.split(jax.random.key(seed), 28)
    return {
        "residual": draw_residual(jax.random.fold_in(seeds[27], 71), 0),
        "first_gain": jnp.clip(1.0 + 0.18 * jax.random.normal(seeds[1], (D,), jnp.float32), 0.099609375, 1.8984375).astype(jnp.bfloat16),
        "first_gate": gaussian(seeds[2], (D, FF), D ** -0.5, 0.125, ((0, 4), (1, 8))),
        "first_lift": gaussian(seeds[3], (D, FF), D ** -0.5, 0.125, ((0, 4), (1, 8))),
        "first_down": gaussian(seeds[4], (FF, D), FF ** -0.5, 0.078125, ((0, 8), (1, 4))),
        "mixer_gain": jnp.clip(1.0 + 0.18 * jax.random.normal(seeds[5], (D,), jnp.float32), 0.099609375, 1.8984375).astype(jnp.bfloat16),
        "proj_gate": gaussian(seeds[6], (D, D_SSD), D ** -0.5, 0.125, ((1, 4),)),
        "proj_input": gaussian(seeds[7], (D, D_SSD), D ** -0.5, 0.125, ((1, 4),)),
        "proj_write": gaussian(seeds[8], (D, NGROUPS * STATE), D ** -0.5, 0.125, ((1, 4),)),
        "proj_read": gaussian(seeds[9], (D, NGROUPS * STATE), D ** -0.5, 0.125, ((1, 4),)),
        "proj_step": gaussian(seeds[10], (D, HEADS), D ** -0.5, 0.125, ((1, 4),)),
        "step_bias": jnp.clip(-5.0 + 3.0 * jax.random.uniform(seeds[11], (HEADS,), jnp.float32) ** steps_of(seeds[11], (HEADS,), ((0, 4),), -0.2, 0.2), -5.0, -2.0),
        "rate_log": jnp.clip(-0.7 + 2.8 * jax.random.uniform(seeds[12], (HEADS,), jnp.float32) ** steps_of(seeds[12], (HEADS,), ((0, 4),), -0.2, 0.2), -0.7, 2.1),
        "skip_gain": jnp.clip(0.5 + 1.5 * jax.random.uniform(seeds[13], (HEADS,), jnp.float32) ** steps_of(seeds[13], (HEADS,), ((0, 4),), -0.2, 0.2), 0.5, 2.0),
        "taps_input": gaussian(seeds[14], (CONV, D_SSD), CONV ** -0.5, 3.0, ((1, 4),)),
        "taps_write": gaussian(seeds[15], (CONV, NGROUPS * STATE), CONV ** -0.5, 3.0, ((1, 4),)),
        "taps_read": gaussian(seeds[16], (CONV, NGROUPS * STATE), CONV ** -0.5, 3.0, ((1, 4),)),
        "buffer_input": gaussian(seeds[17], (BATCH, CONV - 1, D_SSD), 1.0, 6.0, ((0, 8), (2, 4))),
        "buffer_write": gaussian(seeds[18], (BATCH, CONV - 1, NGROUPS * STATE), 1.0, 6.0, ((0, 8), (2, 4))),
        "buffer_read": gaussian(seeds[19], (BATCH, CONV - 1, NGROUPS * STATE), 1.0, 6.0, ((0, 8), (2, 4))),
        "scan_state": gaussian(seeds[20], (BATCH, HEADS, HEAD_DIM, STATE), 0.1, 1.5, ((0, 8), (1, 4)), jnp.float32),
        "group_gain": jnp.clip(1.0 + 0.18 * jax.random.normal(seeds[21], (D_SSD,), jnp.float32), 0.099609375, 1.8984375).astype(jnp.bfloat16),
        "proj_output": gaussian(seeds[22], (D_SSD, D), D_SSD ** -0.5, 0.125, ((0, 4),)),
        "second_gain": jnp.clip(1.0 + 0.18 * jax.random.normal(seeds[23], (D,), jnp.float32), 0.099609375, 1.8984375).astype(jnp.bfloat16),
        "second_gate": gaussian(seeds[24], (D, FF), D ** -0.5, 0.125, ((0, 4), (1, 8))),
        "second_lift": gaussian(seeds[25], (D, FF), D ** -0.5, 0.125, ((0, 4), (1, 8))),
        "second_down": gaussian(seeds[26], (FF, D), FF ** -0.5, 0.078125, ((0, 8), (1, 4))),
    }


norm_eps = 1e-06

def inverse_rms(values):
    return lax.rsqrt(lax.optimization_barrier(jnp.mean(values * values, axis=-1, keepdims=True)) + norm_eps)

def block_sum(activ, weight, pieces):
    seq_rows = activ.shape[0]
    inner = activ.shape[1] // pieces
    widened = lax.optimization_barrier(activ).astype(jnp.float32).reshape(seq_rows, pieces, inner)
    weight_f = weight.astype(jnp.float32).reshape(pieces, inner, weight.shape[1])
    partial_value = jnp.einsum('btk,tkf->tbf', widened, weight_f)
    rounded = lax.optimization_barrier(partial_value.astype(jnp.bfloat16)).astype(jnp.float32)
    return lax.optimization_barrier(jnp.sum(rounded, axis=0))

def half_step(residual, gain, gate_weight, lift_weight, down_weight):
    widened = residual.astype(jnp.float32)
    normed = (widened * inverse_rms(widened) * gain.astype(jnp.float32)).astype(jnp.bfloat16)
    gate_sum = block_sum(normed, gate_weight, N_TP)
    up_sum = block_sum(normed, lift_weight, N_TP)
    hidden = (jax.nn.silu(gate_sum) * up_sum).astype(jnp.bfloat16)
    branch = jnp.dot(hidden, down_weight, preferred_element_type=jnp.float32)
    return (widened + 0.5 * branch).astype(jnp.bfloat16)

def short_conv(tap_weights, buffer, newest):
    taps_f = tap_weights.astype(jnp.float32)
    summed = lax.optimization_barrier(jnp.sum(buffer.astype(jnp.float32) * taps_f[None, :-1, :], axis=1))
    summed = summed + newest.astype(jnp.float32) * taps_f[-1][None, :]
    return jax.nn.silu(summed)

def state_mixer(residual, mixer_gain, proj_gate, proj_input, proj_write, proj_read, proj_step, step_bias, rate_log, skip_gain, taps_input, taps_write, taps_read, buffer_input, buffer_write, buffer_read, scan_state, group_gain, proj_output):
    seq_rows = residual.shape[0]
    widened = residual.astype(jnp.float32)
    normed = (widened * inverse_rms(widened) * mixer_gain.astype(jnp.float32)).astype(jnp.bfloat16)

    def project(weight):
        return jnp.dot(normed, weight, preferred_element_type=jnp.float32).astype(jnp.bfloat16)
    gate_z = project(proj_gate)
    input_new = project(proj_input)
    write_new = project(proj_write)
    read_new = project(proj_read)
    step_raw = project(proj_step)
    input_conv = short_conv(taps_input, buffer_input, input_new)
    write_conv = short_conv(taps_write, buffer_write, write_new)
    read_conv = short_conv(taps_read, buffer_read, read_new)
    head_count = proj_step.shape[1]
    group_count = proj_write.shape[1] // STATE
    per_group = head_count // group_count
    step = jax.nn.softplus(step_raw.astype(jnp.float32) + step_bias[None, :])
    retain = jnp.exp(-step * jnp.exp(rate_log)[None, :])
    input_heads = input_conv.reshape(seq_rows, group_count, per_group, HEAD_DIM)
    write_groups = write_conv.reshape(seq_rows, group_count, STATE)
    read_groups = read_conv.reshape(seq_rows, group_count, STATE)
    old_state = scan_state.reshape(seq_rows, group_count, per_group, HEAD_DIM, STATE)
    retain_g = retain.reshape(seq_rows, group_count, per_group)
    step_g = step.reshape(seq_rows, group_count, per_group)
    updated = retain_g[..., None, None] * old_state + (step_g[..., None] * input_heads)[..., None] * write_groups[:, :, None, None, :]
    head_out = jnp.einsum('bgrpn,bgn->bgrp', updated, read_groups, precision=lax.Precision.HIGHEST)
    head_out = head_out + skip_gain.reshape(group_count, per_group)[None, :, :, None] * input_heads
    head_short = lax.optimization_barrier(head_out.astype(jnp.bfloat16))
    gated = head_short.astype(jnp.float32).reshape(seq_rows, group_count, per_group * HEAD_DIM)
    gated = gated * jax.nn.silu(gate_z.astype(jnp.float32).reshape(seq_rows, group_count, per_group * HEAD_DIM))
    gated = gated * inverse_rms(gated) * group_gain.astype(jnp.float32).reshape(group_count, per_group * HEAD_DIM)[None]
    gated = gated.reshape(seq_rows, head_count * HEAD_DIM).astype(jnp.bfloat16)
    mixed = block_sum(gated, proj_output, N_TP)
    return ((widened + mixed).astype(jnp.bfloat16), updated.reshape(seq_rows, head_count, HEAD_DIM, STATE))

def reference(residual, first_gain, first_gate, first_lift, first_down, mixer_gain, proj_gate, proj_input, proj_write, proj_read, proj_step, step_bias, rate_log, skip_gain, taps_input, taps_write, taps_read, buffer_input, buffer_write, buffer_read, scan_state, group_gain, proj_output, second_gain, second_gate, second_lift, second_down):
    first = half_step(residual, first_gain, first_gate, first_lift, first_down)
    mixed, state_out = state_mixer(first, mixer_gain, proj_gate, proj_input, proj_write, proj_read, proj_step, step_bias, rate_log, skip_gain, taps_input, taps_write, taps_read, buffer_input, buffer_write, buffer_read, scan_state, group_gain, proj_output)
    residual_out = half_step(mixed, second_gain, second_gate, second_lift, second_down)
    return (residual_out, state_out)
```

```python
import functools

import jax
import jax.numpy as jnp
from jax import lax
from jax.experimental import pallas as pl
from jax.experimental.pallas import tpu as pltpu
from jax.sharding import PartitionSpec as P

HEAD_DIM = 64
STATE = 128
EPS = 1e-06
MESH = pl.DeviceIdType.MESH
F32 = jnp.float32
BF16 = jnp.bfloat16
VMEM_LIMIT = 60 * 1024 * 1024


def silu(v):
    return v / (1.0 + jnp.exp(-v))


def dot(a, b):
    return jnp.dot(a, b, preferred_element_type=F32)


def enter(nk, nt, kv, tp):
    barrier = pltpu.get_barrier_semaphore()
    for d in range(1, nk):
        pl.semaphore_signal(
            barrier, inc=1, device_id={"kv": lax.rem(kv + d, nk)}, device_id_type=MESH
        )
    for d in range(1, nt):
        pl.semaphore_signal(
            barrier, inc=1, device_id={"tp": lax.rem(tp + d, nt)}, device_id_type=MESH
        )
    pl.semaphore_wait(barrier, nk + nt - 2)


def far_first(n):
    return sorted(range(1, n), key=lambda d: -min(d, n - d))


def remote(src, dst, send, recv, where):
    return pltpu.make_async_remote_copy(
        src_ref=src, dst_ref=dst, send_sem=send, recv_sem=recv,
        device_id=where, device_id_type=MESH,
    )


def half_scratch(nk, nt, rows, width, cols):
    total = nk * rows
    share = total // nt
    dma = pltpu.SemaphoreType.DMA
    return [
        pltpu.VMEM((width, cols), BF16),
        pltpu.VMEM((width, cols), BF16),
        pltpu.VMEM((cols, width), BF16),
        dma((3,)),
        pltpu.VMEM((total, width), BF16),
        pltpu.VMEM((total, width), BF16),
        pltpu.VMEM((total, 128), F32),
        pltpu.VMEM((nt, share, 128), F32),
        pltpu.VMEM((nt, 2, share, cols), BF16),
        pltpu.VMEM((nt, 2, share, cols), BF16),
        pltpu.VMEM((total, cols), BF16),
        pltpu.VMEM((total, width), BF16),
        pltpu.VMEM((nk, rows, width), BF16),
        dma((nk,)), dma((nk,)),
        dma((nt,)), dma((nt,)),
        dma((nt,)), dma((nt,)),
        dma((nt,)), dma((nt,)),
        dma((nk,)), dma((nk,)),
    ]


def start_weights(gate_hbm, lift_hbm, down_hbm, scratch):
    wg, wu, wd, wsem = scratch[:4]
    copies = [
        pltpu.make_async_copy(gate_hbm, wg, wsem.at[0]),
        pltpu.make_async_copy(lift_hbm, wu, wsem.at[1]),
        pltpu.make_async_copy(down_hbm, wd, wsem.at[2]),
    ]
    for c in copies:
        c.start()
    return copies


def half_body(nk, nt, kv, tp, x_ref, gain_ref, weights, scratch):
    (wg, wu, wd, _, xall, xg, ssq, ssr, part, parr, hid, dpart, dparr,
     ag_s, ag_r, sq_s, sq_r, rs_s, rs_r, hg_s, hg_r, dn_s, dn_r) = scratch
    rows, width = x_ref.shape
    total = nk * rows
    share = total // nt
    per = share // rows
    features = width * nt
    sends = []
    gathers = []
    for d in far_first(nk):
        c = remote(x_ref, xall.at[pl.ds(kv * rows, rows)], ag_s.at[d], ag_r.at[d],
                   {"kv": lax.rem(kv + d, nk)})
        c.start()
        gathers.append(c)
    xall[pl.ds(kv * rows, rows), :] = x_ref[...]
    gain = gain_ref[...].astype(F32)
    for c in reversed(gathers):
        c.wait_recv()
    for k in range(nk):
        at = pl.ds(k * rows, rows)
        value = xall[at, :].astype(F32)
        ssq[at, :] = jnp.broadcast_to(
            jnp.sum(value * value, axis=1, keepdims=True), (rows, 128)
        )
        xg[at, :] = (value * gain).astype(BF16)
    squares = []
    for d in far_first(nt):
        to = lax.rem(tp + d, nt)
        c = remote(ssq.at[pl.ds(to * share, share)], ssr.at[d], sq_s.at[d], sq_r.at[d],
                   {"tp": to})
        c.start()
        squares.append(c)
    weights[0].wait()
    weights[1].wait()
    parts = []
    for d in far_first(nt) + [0]:
        to = lax.rem(tp + d, nt)
        a = xg[pl.ds(to * share, share), :]
        part[d, 0] = dot(a, wg[...]).astype(BF16)
        part[d, 1] = dot(a, wu[...]).astype(BF16)
        if d:
            c = remote(part.at[d], parr.at[d], rs_s.at[d], rs_r.at[d], {"tp": to})
            c.start()
            parts.append(c)
    mine = pl.ds(tp * share, share)
    sq = ssq[mine, :]
    for d, c in zip(far_first(nt), squares):
        c.wait_recv()
        sq = sq + ssr[d]
    factor = lax.rsqrt(sq[:, :1] / features + EPS)
    gate = part[0, 0].astype(F32)
    lift = part[0, 1].astype(F32)
    for d, c in reversed(list(zip(far_first(nt), parts))):
        c.wait_recv()
        gate = gate + parr[d, 0].astype(F32)
        lift = lift + parr[d, 1].astype(F32)
    gate = gate * factor
    lift = lift * factor
    hid[mine, :] = (silu(gate) * lift).astype(BF16)
    spread = {}
    for d in far_first(nt):
        c = remote(hid.at[mine], hid.at[mine], hg_s.at[d], hg_r.at[d],
                   {"tp": lax.rem(tp + d, nt)})
        c.start()
        spread[d] = c
    weights[2].wait()
    for d in [0] + list(reversed(far_first(nt))):
        if d:
            spread[d].wait_recv()
        source = lax.rem(tp + nt - d, nt)
        block = pl.ds(source * share, share)
        dpart[block, :] = dot(hid[block, :], wd[...]).astype(BF16)
        for j in range(per):
            to = source * per + j

            @pl.when(to != kv)
            def _():
                remote(dpart.at[pl.ds(to * rows, rows)], dparr.at[kv], dn_s.at[to],
                       dn_r.at[kv], {"kv": to}).start()

    acc = dpart[pl.ds(kv * rows, rows), :].astype(F32)
    for d in reversed(far_first(nk)):
        source = lax.rem(kv + nk - d, nk)
        pltpu.make_async_copy(dparr.at[source], dparr.at[source], dn_r.at[source]).wait()
        acc = acc + dparr[source].astype(F32)
    for d in far_first(nk):
        to = lax.rem(kv + d, nk)
        pltpu.make_async_copy(dparr.at[to], dparr.at[to], dn_s.at[to]).wait()
    for c in gathers + squares + parts + list(spread.values()):
        c.wait_send()
    return (x_ref[...].astype(F32) + 0.5 * acc).astype(BF16)


def first_kernel(nk, nt, x_ref, gain_ref, gate, lift, down, own_ref, all_ref, *scratch):
    kv, tp = lax.axis_index("kv"), lax.axis_index("tp")
    held, f_s, f_r = scratch[:3]
    scratch = scratch[3:]
    weights = start_weights(gate, lift, down, scratch)
    enter(nk, nt, kv, tp)
    out = half_body(nk, nt, kv, tp, x_ref, gain_ref, weights, scratch)
    own_ref[...] = out
    held[tp] = out
    copies = []
    for d in far_first(nt):
        c = remote(held.at[tp], held.at[tp], f_s.at[d], f_r.at[d],
                   {"tp": lax.rem(tp + d, nt)})
        c.start()
        copies.append(c)
    for c in copies:
        c.wait_recv()
    all_ref[...] = held[...]
    for c in copies:
        c.wait_send()


def second_kernel(nk, nt, own_ref, pout_ref, gain_ref, gate, lift, down, out_ref, *scratch):
    kv, tp = lax.axis_index("kv"), lax.axis_index("tp")
    arrived, x_buf, m_s, m_r = scratch[:4]
    scratch = scratch[4:]
    weights = start_weights(gate, lift, down, scratch)
    enter(nk, nt, kv, tp)
    copies = []
    for d in far_first(nt):
        to = lax.rem(tp + d, nt)
        c = remote(pout_ref.at[to], arrived.at[d], m_s.at[d], m_r.at[d], {"tp": to})
        c.start()
        copies.append(c)
    acc = own_ref[...].astype(F32) + pout_ref[tp].astype(F32)
    for d, c in zip(far_first(nt), copies):
        c.wait_recv()
        acc = acc + arrived[d].astype(F32)
    x_buf[...] = acc.astype(BF16)
    out_ref[...] = half_body(nk, nt, kv, tp, x_buf, gain_ref, weights, scratch)
    for c in copies:
        c.wait_send()


def vmem(n):
    return [pl.BlockSpec(memory_space=pltpu.VMEM)] * n


def params(cid):
    return pltpu.CompilerParams(
        collective_id=cid, has_side_effects=True, vmem_limit_bytes=VMEM_LIMIT
    )


def first_half(nk, nt, x, gain, gate, lift, down):
    rows, width = x.shape
    dma = pltpu.SemaphoreType.DMA
    return pl.pallas_call(
        functools.partial(first_kernel, nk, nt),
        out_shape=(jax.ShapeDtypeStruct(x.shape, BF16),
                   jax.ShapeDtypeStruct((nt, rows, width), BF16)),
        in_specs=vmem(2) + [pl.BlockSpec(memory_space=pl.ANY)] * 3,
        out_specs=tuple(vmem(2)),
        scratch_shapes=[pltpu.VMEM((nt, rows, width), BF16), dma((nt,)), dma((nt,))]
        + half_scratch(nk, nt, rows, width, gate.shape[1]),
        compiler_params=params(1),
        name="first_half",
    )(x, gain[None, :], gate, lift, down)


def second_half(nk, nt, own, pout, gain, gate, lift, down):
    rows, width = own.shape
    dma = pltpu.SemaphoreType.DMA
    return pl.pallas_call(
        functools.partial(second_kernel, nk, nt),
        out_shape=jax.ShapeDtypeStruct(own.shape, BF16),
        in_specs=vmem(3) + [pl.BlockSpec(memory_space=pl.ANY)] * 3,
        out_specs=vmem(1)[0],
        scratch_shapes=[pltpu.VMEM((nt, rows, width), BF16), pltpu.VMEM((rows, width), BF16),
                        dma((nt,)), dma((nt,))]
        + half_scratch(nk, nt, rows, width, gate.shape[1]),
        compiler_params=params(2),
        name="second_half",
    )(own, pout, gain[None, :], gate, lift, down)


def conv(taps_ref, buf_ref, newest):
    taps = taps_ref[...].astype(F32)
    count = taps.shape[0]
    old = buf_ref[...].astype(F32)
    acc = newest.astype(BF16).astype(F32) * taps[count - 1 : count]
    for k in range(count - 1):
        acc = acc + old[k] * taps[k : k + 1]
    return silu(acc)


def split(v):
    high = v.astype(BF16).astype(F32)
    return high, v - high


def mixer_kernel(first, gain, wz, wx, wb, wr, ws, bias, rate, skip, tx, tb, tr, bx, bb, br,
                 ggain, wo, state, pout, state_out,
                 z_s, x_s, r_s, ho_s, left_s, base_s):
    step_id = pl.program_id(0)
    nt, rows, width = first.shape
    features = nt * width
    chans = wx.shape[1]
    heads = ws.shape[1]
    groups = wb.shape[1] // STATE
    gch = chans // groups
    depth = base_s.shape[1]

    def spread(v):
        r = lax.broadcasted_iota(jnp.int32, (heads, chans), 0)
        c = lax.broadcasted_iota(jnp.int32, (heads, chans), 1)
        ind = jnp.where(c // HEAD_DIM == r, 1.0, 0.0).astype(F32)
        return jnp.dot(v, ind, precision=lax.Precision.HIGHEST, preferred_element_type=F32)

    @pl.when(step_id == 0)
    def _():
        total = jnp.zeros((rows, 1), F32)
        for t in range(nt):
            v = first[t].astype(F32)
            total = total + jnp.sum(v * v, axis=1, keepdims=True)
        factor = lax.rsqrt(total / features + EPS)
        normed = jnp.concatenate(
            [(first[t].astype(F32) * factor
              * gain[:, t * width:(t + 1) * width].astype(F32)).astype(BF16)
             for t in range(nt)], axis=1)
        z_s[...] = dot(normed, wz[...]).astype(BF16).astype(F32)
        xc = conv(tx, bx, dot(normed, wx[...]))
        x_s[...] = xc
        bc = conv(tb, bb, dot(normed, wb[...]))
        rc = conv(tr, br, dot(normed, wr[...]))
        for i in range(rows):
            r_s[i] = rc[i:i + 1]
        raw = dot(normed, ws[...]).astype(BF16).astype(F32) + bias[...]
        step = jnp.maximum(raw, 0.0) + jnp.log1p(jnp.exp(-jnp.abs(raw)))
        retain = jnp.exp(-step * jnp.exp(rate[...]))
        sx_hi, sx_lo = split(spread(step) * xc)
        re_hi, re_lo = split(spread(retain))
        pad = depth - 5 * rows
        left = jnp.concatenate(
            [sx_hi, sx_lo, sx_hi, re_hi, re_lo, jnp.zeros((pad, chans), F32)], axis=0)
        left_s[...] = left.T.astype(BF16)
        for g in range(groups):
            b_hi, b_lo = split(bc[:, g * STATE:(g + 1) * STATE])
            zero = jnp.zeros((rows, STATE), F32)
            one = jnp.ones((rows, STATE), F32)
            zpad = jnp.zeros((pad, STATE), F32)
            base_s[g, :, :STATE] = jnp.concatenate(
                [b_hi, b_hi, b_lo, zero, zero, zpad], axis=0)
            base_s[g, :, STATE:] = jnp.concatenate(
                [zero, zero, zero, one, one, zpad], axis=0)

    block = state.shape[0]
    rowmod = lax.rem(lax.broadcasted_iota(jnp.int32, (depth, 2 * STATE), 0), rows)
    pick = lax.broadcasted_iota(jnp.int32, (16, STATE), 0)
    hg = heads // groups
    for i in range(block):
        b = step_id * block + i
        for g in range(groups):
            right = jnp.where(rowmod == b, base_s[g], 0.0).astype(BF16)
            both = dot(left_s[g * gch:(g + 1) * gch, :], right)
            old = state[i, g * hg:(g + 1) * hg].reshape(gch, STATE)
            new = both[:, STATE:] * old + both[:, :STATE]
            state_out[i, g * hg:(g + 1) * hg] = new.reshape(hg, HEAD_DIM, STATE)
            r_hi, r_lo = split(r_s[b][:, g * STATE:(g + 1) * STATE])
            rr = jnp.where(pick == 0, r_hi, jnp.where(pick == 1, r_lo, 0.0)).astype(BF16)
            ho = lax.dot_general(rr, new.astype(BF16), (((1,), (1,)), ((), ())),
                                 preferred_element_type=F32)
            ho_s[b, :, g * gch:(g + 1) * gch] = jnp.sum(ho, axis=0, keepdims=True)

    @pl.when(step_id == pl.num_programs(0) - 1)
    def _():
        heads_out = jnp.concatenate([ho_s[i] for i in range(rows)], axis=0)
        out = (heads_out + spread(skip[...]) * x_s[...]).astype(BF16).astype(F32)
        gated = out * silu(z_s[...])
        pieces = []
        for g in range(groups):
            v = gated[:, g * gch:(g + 1) * gch]
            pieces.append(v * lax.rsqrt(jnp.mean(v * v, axis=1, keepdims=True) + EPS))
        gated = (jnp.concatenate(pieces, axis=1) * ggain[...].astype(F32)).astype(BF16)
        for t in range(nt):
            pout[t] = dot(gated, wo[:, t * width:(t + 1) * width]).astype(BF16)


def mixer(first, gain, wz, wx, wb, wr, ws, bias, rate, skip, tx, tb, tr, bx, bb, br,
          state, ggain, wo):
    nt, rows, width = first.shape
    chans, heads = wx.shape[1], ws.shape[1]
    groups = wb.shape[1] // STATE
    depth = -(-5 * rows // 128) * 128
    block = 4 if rows % 4 == 0 else 1
    small = [first, gain[None, :], wz, wx, wb, wr, ws, bias[None, :], rate[None, :],
             skip[None, :], tx, tb, tr] + [jnp.transpose(v, (1, 0, 2)) for v in (bx, bb, br)] + [
             ggain[None, :], wo]

    def whole(v):
        zeros = (0,) * v.ndim
        return pl.BlockSpec(v.shape, lambda i: zeros, pipeline_mode=pl.Buffered(1))

    state_spec = pl.BlockSpec((block,) + state.shape[1:], lambda i: (i, 0, 0, 0))
    return pl.pallas_call(
        mixer_kernel,
        grid=(rows // block,),
        out_shape=(jax.ShapeDtypeStruct(first.shape, BF16),
                   jax.ShapeDtypeStruct(state.shape, F32)),
        in_specs=[whole(v) for v in small] + [state_spec],
        out_specs=(pl.BlockSpec(first.shape, lambda i: (0, 0, 0)), state_spec),
        scratch_shapes=[
            pltpu.VMEM((rows, chans), F32),
            pltpu.VMEM((rows, chans), F32),
            pltpu.VMEM((rows, 1, groups * STATE), F32),
            pltpu.VMEM((rows, 1, chans), F32),
            pltpu.VMEM((chans, depth), BF16),
            pltpu.VMEM((groups, depth, 2 * STATE), F32),
        ],
        compiler_params=pltpu.CompilerParams(
            vmem_limit_bytes=VMEM_LIMIT, dimension_semantics=("arbitrary",)),
        name="mixer",
    )(*small, state)


def per_device(nk, nt, residual, first_gain, first_gate, first_lift, first_down, *rest):
    mix = rest[:18]
    second_gain, second_gate, second_lift, second_down = rest[18:]
    own, gathered = first_half(nk, nt, residual, first_gain, first_gate, first_lift, first_down)
    pout, state_out = mixer(gathered, *mix)
    out = second_half(nk, nt, own, pout, second_gain, second_gate, second_lift, second_down)
    return (out, state_out)


def solution(mesh):
    placed = (
        P("kv", "tp"),
        P("tp"),
        P("tp", "kv"),
        P("tp", "kv"),
        P("kv", "tp"),
        P(),
        P(None, "tp"),
        P(None, "tp"),
        P(None, "tp"),
        P(None, "tp"),
        P(None, "tp"),
        P("tp"),
        P("tp"),
        P("tp"),
        P(None, "tp"),
        P(None, "tp"),
        P(None, "tp"),
        P("kv", None, "tp"),
        P("kv", None, "tp"),
        P("kv", None, "tp"),
        P("kv", "tp", None, None),
        P("tp"),
        P("tp", None),
        P("tp"),
        P("tp", "kv"),
        P("tp", "kv"),
        P("kv", "tp"),
    )
    return jax.shard_map(
        functools.partial(per_device, mesh.shape["kv"], mesh.shape["tp"]),
        mesh=mesh,
        in_specs=placed,
        out_specs=(P("kv", "tp"), P("kv", "tp", None, None)),
        check_vma=False,
    )
```

```python
import functools

import jax
import jax.numpy as jnp
from jax import lax
from jax.experimental import pallas as pl
from jax.experimental.pallas import tpu as pltpu
from jax.sharding import PartitionSpec as P

HEAD_DIM = 64
STATE = 128
EPS = 1e-06
MESH = pl.DeviceIdType.MESH
F32 = jnp.float32
BF16 = jnp.bfloat16
VMEM_LIMIT = 60 * 1024 * 1024


def silu(v):
    return v / (1.0 + jnp.exp(-v))


def dot(a, b):
    return jnp.dot(a, b, preferred_element_type=F32)


def dot_t(a, b):
    return lax.dot_general(a, b, (((1,), (1,)), ((), ())), preferred_element_type=F32)


def enter(nk, nt, kv, tp):
    barrier = pltpu.get_barrier_semaphore()
    for d in range(1, nk):
        pl.semaphore_signal(
            barrier, inc=1, device_id={"kv": lax.rem(kv + d, nk)}, device_id_type=MESH
        )
    for d in range(1, nt):
        pl.semaphore_signal(
            barrier, inc=1, device_id={"tp": lax.rem(tp + d, nt)}, device_id_type=MESH
        )
    pl.semaphore_wait(barrier, nk + nt - 2)


def far_first(n):
    return sorted(range(1, n), key=lambda d: -min(d, n - d))


def remote(src, dst, send, recv, where):
    return pltpu.make_async_remote_copy(
        src_ref=src, dst_ref=dst, send_sem=send, recv_sem=recv,
        device_id=where, device_id_type=MESH,
    )


def half_scratch(nk, nt, rows, width, cols):
    total = nk * rows
    share = total // nt
    dma = pltpu.SemaphoreType.DMA
    return [
        pltpu.VMEM((cols, width), BF16),
        pltpu.VMEM((cols, width), BF16),
        pltpu.VMEM((cols, width), BF16),
        dma((3,)),
        pltpu.VMEM((total, width), BF16),
        pltpu.VMEM((total, width), BF16),
        pltpu.VMEM((total, 128), F32),
        pltpu.VMEM((nt, share, 128), F32),
        pltpu.VMEM((nt, 2, share, cols), BF16),
        pltpu.VMEM((nt, 2, share, cols), BF16),
        pltpu.VMEM((total, cols), BF16),
        pltpu.VMEM((total, width), BF16),
        pltpu.VMEM((nk, rows, width), BF16),
        dma((nk,)), dma((nk,)),
        dma((nt,)), dma((nt,)),
        dma((nt,)), dma((nt,)),
        dma((nt,)), dma((nt,)),
        dma((nk,)), dma((nk,)),
    ]


def start_weights(gate_hbm, lift_hbm, down_hbm, scratch):
    wg, wu, wd, wsem = scratch[:4]
    copies = [
        pltpu.make_async_copy(gate_hbm, wg, wsem.at[0]),
        pltpu.make_async_copy(lift_hbm, wu, wsem.at[1]),
        pltpu.make_async_copy(down_hbm, wd, wsem.at[2]),
    ]
    for c in copies:
        c.start()
    return copies


def half_body(nk, nt, kv, tp, place, x_ref, gain_ref, weights, scratch):
    (wg, wu, wd, _, xall, xg, ssq, ssr, part, parr, hid, dpart, dparr,
     ag_s, ag_r, sq_s, sq_r, rs_s, rs_r, hg_s, hg_r, dn_s, dn_r) = scratch
    rows, width = x_ref.shape
    total = nk * rows
    share = total // nt
    per = share // rows
    features = width * nt
    sends = []
    gathers = []
    for d in far_first(nk):
        c = remote(x_ref, xall.at[pl.ds(kv * rows, rows)], ag_s.at[d], ag_r.at[d],
                   {"kv": lax.rem(kv + d, nk)})
        c.start()
        gathers.append(c)
    xall[pl.ds(kv * rows, rows), :] = x_ref[...]
    gain = gain_ref[:, place * width:(place + 1) * width].astype(F32)
    for c in reversed(gathers):
        c.wait_recv()
    for k in range(nk):
        at = pl.ds(k * rows, rows)
        value = xall[at, :].astype(F32)
        ssq[at, :] = jnp.broadcast_to(
            jnp.sum(value * value, axis=1, keepdims=True), (rows, 128)
        )
        xg[at, :] = (value * gain).astype(BF16)
    squares = []
    for d in far_first(nt):
        to = lax.rem(tp + d, nt)
        c = remote(ssq.at[pl.ds(to * share, share)], ssr.at[d], sq_s.at[d], sq_r.at[d],
                   {"tp": to})
        c.start()
        squares.append(c)
    weights[0].wait()
    weights[1].wait()
    parts = []
    for d in far_first(nt) + [0]:
        to = lax.rem(tp + d, nt)
        a = xg[pl.ds(to * share, share), :]
        part[d, 0] = dot_t(a, wg[...]).astype(BF16)
        part[d, 1] = dot_t(a, wu[...]).astype(BF16)
        if d:
            c = remote(part.at[d], parr.at[d], rs_s.at[d], rs_r.at[d], {"tp": to})
            c.start()
            parts.append(c)
    mine = pl.ds(tp * share, share)
    sq = ssq[mine, :]
    for d, c in zip(far_first(nt), squares):
        c.wait_recv()
        sq = sq + ssr[d]
    factor = lax.rsqrt(sq[:, :1] / features + EPS)
    gate = part[0, 0].astype(F32)
    lift = part[0, 1].astype(F32)
    for d, c in reversed(list(zip(far_first(nt), parts))):
        c.wait_recv()
        gate = gate + parr[d, 0].astype(F32)
        lift = lift + parr[d, 1].astype(F32)
    gate = gate * factor
    lift = lift * factor
    hid[mine, :] = (silu(gate) * lift).astype(BF16)
    spread = {}
    for d in far_first(nt):
        c = remote(hid.at[mine], hid.at[mine], hg_s.at[d], hg_r.at[d],
                   {"tp": lax.rem(tp + d, nt)})
        c.start()
        spread[d] = c
    weights[2].wait()
    for d in [0] + list(reversed(far_first(nt))):
        if d:
            spread[d].wait_recv()
        source = lax.rem(tp + nt - d, nt)
        block = pl.ds(source * share, share)
        dpart[block, :] = dot(hid[block, :], wd[...]).astype(BF16)
        for j in range(per):
            to = source * per + j

            @pl.when(to != kv)
            def _():
                remote(dpart.at[pl.ds(to * rows, rows)], dparr.at[kv], dn_s.at[to],
                       dn_r.at[kv], {"kv": to}).start()

    acc = dpart[pl.ds(kv * rows, rows), :].astype(F32)
    for d in reversed(far_first(nk)):
        source = lax.rem(kv + nk - d, nk)
        pltpu.make_async_copy(dparr.at[source], dparr.at[source], dn_r.at[source]).wait()
        acc = acc + dparr[source].astype(F32)
    for d in far_first(nk):
        to = lax.rem(kv + d, nk)
        pltpu.make_async_copy(dparr.at[to], dparr.at[to], dn_s.at[to]).wait()
    for c in gathers + squares + parts + list(spread.values()):
        c.wait_send()
    return (x_ref[...].astype(F32) + 0.5 * acc).astype(BF16)


def first_kernel(nk, nt, x_ref, gain_ref, gate, lift, down, own_ref, all_ref, *scratch):
    kv, tp = lax.axis_index("kv"), lax.axis_index("tp")
    held, f_s, f_r = scratch[:3]
    scratch = scratch[3:]
    weights = start_weights(gate, lift, down, scratch)
    enter(nk, nt, kv, tp)
    out = half_body(nk, nt, kv, tp, 0, x_ref, gain_ref, weights, scratch)
    own_ref[...] = out
    held[tp] = out
    copies = []
    for d in far_first(nt):
        c = remote(held.at[tp], held.at[tp], f_s.at[d], f_r.at[d],
                   {"tp": lax.rem(tp + d, nt)})
        c.start()
        copies.append(c)
    for c in copies:
        c.wait_recv()
    all_ref[...] = held[...]
    for c in copies:
        c.wait_send()


def second_kernel(nk, nt, own_ref, pout_ref, gain_ref, gate, lift, down, out_ref, *scratch):
    kv, tp = lax.axis_index("kv"), lax.axis_index("tp")
    arrived, x_buf, m_s, m_r = scratch[:4]
    scratch = scratch[4:]
    weights = start_weights(gate, lift, down, scratch)
    enter(nk, nt, kv, tp)
    copies = []
    for d in far_first(nt):
        to = lax.rem(tp + d, nt)
        c = remote(pout_ref.at[to], arrived.at[d], m_s.at[d], m_r.at[d], {"tp": to})
        c.start()
        copies.append(c)
    acc = own_ref[...].astype(F32) + pout_ref[tp].astype(F32)
    for d, c in zip(far_first(nt), copies):
        c.wait_recv()
        acc = acc + arrived[d].astype(F32)
    x_buf[...] = acc.astype(BF16)
    out_ref[...] = half_body(nk, nt, kv, tp, 1, x_buf, gain_ref, weights, scratch)
    for c in copies:
        c.wait_send()


def vmem(n):
    return [pl.BlockSpec(memory_space=pltpu.VMEM)] * n


def params(cid):
    return pltpu.CompilerParams(
        collective_id=cid, has_side_effects=True, vmem_limit_bytes=VMEM_LIMIT
    )


def first_half(nk, nt, x, gain, gate, lift, down):
    rows, width = x.shape
    dma = pltpu.SemaphoreType.DMA
    return pl.pallas_call(
        functools.partial(first_kernel, nk, nt),
        out_shape=(jax.ShapeDtypeStruct(x.shape, BF16),
                   jax.ShapeDtypeStruct((nt, rows, width), BF16)),
        in_specs=vmem(2) + [pl.BlockSpec(memory_space=pl.ANY)] * 3,
        out_specs=tuple(vmem(2)),
        scratch_shapes=[pltpu.VMEM((nt, rows, width), BF16), dma((nt,)), dma((nt,))]
        + half_scratch(nk, nt, rows, width, gate.shape[0]),
        compiler_params=params(1),
        name="first_half",
    )(x, gain, gate, lift, down)


def second_half(nk, nt, own, pout, gain, gate, lift, down):
    rows, width = own.shape
    dma = pltpu.SemaphoreType.DMA
    return pl.pallas_call(
        functools.partial(second_kernel, nk, nt),
        out_shape=jax.ShapeDtypeStruct(own.shape, BF16),
        in_specs=vmem(3) + [pl.BlockSpec(memory_space=pl.ANY)] * 3,
        out_specs=vmem(1)[0],
        scratch_shapes=[pltpu.VMEM((nt, rows, width), BF16), pltpu.VMEM((rows, width), BF16),
                        dma((nt,)), dma((nt,))]
        + half_scratch(nk, nt, rows, width, gate.shape[0]),
        compiler_params=params(2),
        name="second_half",
    )(own, pout, gain, gate, lift, down)


def conv(taps_ref, buf_ref, newest):
    taps = taps_ref[...].astype(F32)
    count = taps.shape[0]
    old = buf_ref[...].astype(F32)
    acc = newest.astype(BF16).astype(F32) * taps[count - 1 : count]
    for k in range(count - 1):
        acc = acc + old[k] * taps[k : k + 1]
    return silu(acc)


def split(v):
    high = v.astype(BF16).astype(F32)
    return high, v - high


def mixer_kernel(first, gain, wz, wx, wb, wr, ws, bias, rate, skip, tx, tb, tr, bx, bb, br,
                 wo, state, pout, state_out,
                 z_s, x_s, r_s, ho_s, left_s, base_s):
    step_id = pl.program_id(0)
    nt, rows, width = first.shape
    features = nt * width
    chans = wx.shape[1]
    heads = ws.shape[0]
    groups = wb.shape[1] // STATE
    gch = chans // groups
    depth = base_s.shape[1]

    def spread(v):
        r = lax.broadcasted_iota(jnp.int32, (heads, chans), 0)
        c = lax.broadcasted_iota(jnp.int32, (heads, chans), 1)
        ind = jnp.where(c // HEAD_DIM == r, 1.0, 0.0).astype(F32)
        return jnp.dot(v, ind, precision=lax.Precision.HIGHEST, preferred_element_type=F32)

    @pl.when(step_id == 0)
    def _():
        total = jnp.zeros((rows, 1), F32)
        for t in range(nt):
            v = first[t].astype(F32)
            total = total + jnp.sum(v * v, axis=1, keepdims=True)
        factor = lax.rsqrt(total / features + EPS)
        normed = jnp.concatenate(
            [(first[t].astype(F32) * factor
              * gain[:, (t + 3) * width:(t + 4) * width].astype(F32)).astype(BF16)
             for t in range(nt)], axis=1)
        z_s[...] = dot(normed, wz[...]).astype(BF16).astype(F32)
        xc = conv(tx, bx, dot(normed, wx[...]))
        x_s[...] = xc
        bc = conv(tb, bb, dot(normed, wb[...]))
        rc = conv(tr, br, dot(normed, wr[...]))
        for i in range(rows):
            r_s[i] = rc[i:i + 1]
        raw = dot_t(normed, ws[...]).astype(BF16).astype(F32) + bias[...]
        step = jnp.maximum(raw, 0.0) + jnp.log1p(jnp.exp(-jnp.abs(raw)))
        retain = jnp.exp(-step * jnp.exp(rate[...]))
        sx_hi, sx_lo = split(spread(step) * xc)
        re_hi, re_lo = split(spread(retain))
        pad = depth - 5 * rows
        left = jnp.concatenate(
            [sx_hi, sx_lo, sx_hi, re_hi, re_lo, jnp.zeros((pad, chans), F32)], axis=0)
        left_s[...] = left.T.astype(BF16)
        for g in range(groups):
            b_hi, b_lo = split(bc[:, g * STATE:(g + 1) * STATE])
            zero = jnp.zeros((rows, STATE), F32)
            one = jnp.ones((rows, STATE), F32)
            zpad = jnp.zeros((pad, STATE), F32)
            base_s[g, :, :STATE] = jnp.concatenate(
                [b_hi, b_hi, b_lo, zero, zero, zpad], axis=0).astype(BF16)
            base_s[g, :, STATE:] = jnp.concatenate(
                [zero, zero, zero, one, one, zpad], axis=0).astype(BF16)

    block = state.shape[0]
    rowmod = lax.rem(lax.broadcasted_iota(jnp.int32, (depth, 2 * STATE), 0), rows)
    pick = lax.broadcasted_iota(jnp.int32, (16, STATE), 0)
    hg = heads // groups
    for i in range(block):
        b = step_id * block + i
        mask = jnp.where(rowmod == b, 1.0, 0.0).astype(BF16)
        for g in range(groups):
            right = base_s[g] * mask
            both = dot(left_s[g * gch:(g + 1) * gch, :], right)
            old = state[i, g * hg:(g + 1) * hg].reshape(gch, STATE)
            new = both[:, STATE:] * old + both[:, :STATE]
            state_out[i, g * hg:(g + 1) * hg] = new.reshape(hg, HEAD_DIM, STATE)
            r_hi, r_lo = split(r_s[b][:, g * STATE:(g + 1) * STATE])
            rr = jnp.where(pick == 0, r_hi, jnp.where(pick == 1, r_lo, 0.0)).astype(BF16)
            ho = lax.dot_general(rr, new.astype(BF16), (((1,), (1,)), ((), ())),
                                 preferred_element_type=F32)
            ho_s[b, :, g * gch:(g + 1) * gch] = jnp.sum(ho, axis=0, keepdims=True)

    @pl.when(step_id == pl.num_programs(0) - 1)
    def _():
        heads_out = jnp.concatenate([ho_s[i] for i in range(rows)], axis=0)
        out = (heads_out + spread(skip[...]) * x_s[...]).astype(BF16).astype(F32)
        gated = out * silu(z_s[...])
        pieces = []
        for g in range(groups):
            v = gated[:, g * gch:(g + 1) * gch]
            pieces.append(v * lax.rsqrt(jnp.mean(v * v, axis=1, keepdims=True) + EPS))
        gated = (jnp.concatenate(pieces, axis=1) * gain[:, 2 * width:3 * width].astype(F32)).astype(BF16)
        for t in range(nt):
            pout[t] = dot(gated, wo[:, t * width:(t + 1) * width]).astype(BF16)


def mixer(first, gain, wz, wx, wb, wr, ws, bias, rate, skip, tx, tb, tr, bx, bb, br,
          state, wo):
    nt, rows, width = first.shape
    chans, heads = wx.shape[1], ws.shape[0]
    groups = wb.shape[1] // STATE
    depth = -(-5 * rows // 128) * 128
    block = 4 if rows % 4 == 0 else 1
    small = [first, gain, wz, wx, wb, wr, ws, bias[None, :], rate[None, :],
             skip[None, :], tx, tb, tr] + [jnp.transpose(v, (1, 0, 2)) for v in (bx, bb, br)] + [
             wo]

    def whole(v):
        zeros = (0,) * v.ndim
        return pl.BlockSpec(v.shape, lambda i: zeros, pipeline_mode=pl.Buffered(1))

    state_spec = pl.BlockSpec((block,) + state.shape[1:], lambda i: (i, 0, 0, 0))
    return pl.pallas_call(
        mixer_kernel,
        grid=(rows // block,),
        out_shape=(jax.ShapeDtypeStruct(first.shape, BF16),
                   jax.ShapeDtypeStruct(state.shape, F32)),
        in_specs=[whole(v) for v in small] + [state_spec],
        out_specs=(pl.BlockSpec(first.shape, lambda i: (0, 0, 0)), state_spec),
        scratch_shapes=[
            pltpu.VMEM((rows, chans), F32),
            pltpu.VMEM((rows, chans), F32),
            pltpu.VMEM((rows, 1, groups * STATE), F32),
            pltpu.VMEM((rows, 1, chans), F32),
            pltpu.VMEM((chans, depth), BF16),
            pltpu.VMEM((groups, depth, 2 * STATE), BF16),
        ],
        compiler_params=pltpu.CompilerParams(
            vmem_limit_bytes=VMEM_LIMIT, dimension_semantics=("arbitrary",)),
        name="mixer",
    )(*small, state)


def per_device(nk, nt, residual, first_gain, first_gate, first_lift, first_down, *rest):
    mix = list(rest[:18])
    second_gain, second_gate, second_lift, second_down = rest[18:]
    width = residual.shape[1]
    gains = lax.optimization_barrier(
        jnp.concatenate([first_gain, second_gain, mix[16], mix[0]])[None, :])
    mix[0] = gains
    del mix[16]
    mix[5] = mix[5].T
    own, gathered = first_half(
        nk, nt, residual, gains, first_gate.T, first_lift.T, first_down)
    pout, state_out = mixer(gathered, *mix)
    out = second_half(nk, nt, own, pout, gains,
                      second_gate.T, second_lift.T, second_down)
    return (out, state_out)


def solution(mesh):
    placed = (
        P("kv", "tp"),
        P("tp"),
        P("tp", "kv"),
        P("tp", "kv"),
        P("kv", "tp"),
        P(),
        P(None, "tp"),
        P(None, "tp"),
        P(None, "tp"),
        P(None, "tp"),
        P(None, "tp"),
        P("tp"),
        P("tp"),
        P("tp"),
        P(None, "tp"),
        P(None, "tp"),
        P(None, "tp"),
        P("kv", None, "tp"),
        P("kv", None, "tp"),
        P("kv", None, "tp"),
        P("kv", "tp", None, None),
        P("tp"),
        P("tp", None),
        P("tp"),
        P("tp", "kv"),
        P("tp", "kv"),
        P("kv", "tp"),
    )
    return jax.shard_map(
        functools.partial(per_device, mesh.shape["kv"], mesh.shape["tp"]),
        mesh=mesh,
        in_specs=placed,
        out_specs=(P("kv", "tp"), P("kv", "tp", None, None)),
        check_vma=False,
    )
```
